32 devices in a mesh: rep: 2 (over x), fs: 8 (over z, y), tp: 2 (over core).
Axes of the slice: x: 2, y: 2, z: 4, core: 2. Of those that a mesh axis runs over, the one named last changes fastest.
Arguments:
- tokens: bfloat16 [5120, 2048], P(('rep', 'fs'), 'tp'), may hold values from -30 to 30
- mixer_gain: float32 [2048], P('tp'), may hold values from 0.1 to 1.9
- outer_weight: float32 [2048, 1024], P('fs', 'tp'), may hold values from -0.125 to 0.125
- inner_weight: float32 [2048, 1024], P('fs', 'tp'), may hold values from -0.125 to 0.125
- value_weight: float32 [2048, 1024], P('fs', 'tp'), may hold values from -0.125 to 0.125
- outer_scale: float32 [1024], P(('tp', 'fs')), may hold values from 0.5 to 2
- inner_scale: float32 [1024], P(('tp', 'fs')), may hold values from 0.5 to 2
- value_scale: float32 [1024], P(('tp', 'fs')), may hold values from 0.5 to 2
- mixer_taps: float32 [3, 1024], P(None, 'tp'), may hold values from -3.5 to 3.5
- mixer_project: float32 [1024, 2048], P('tp', 'fs'), may hold values from -0.1875 to 0.1875
- project_scale: float32 [2048], P('fs'), may hold values from 0.5 to 2
- channel_gain: float32 [2048], P('tp'), may hold values from 0.1 to 1.9
- gate_weight: float32 [2048, 5632], P('fs', 'tp'), may hold values from -0.125 to 0.125
- gate_scale: float32 [5632], P(('tp', 'fs')), may hold values from 0.5 to 2
- up_weight: float32 [2048, 5632], P('fs', 'tp'), may hold values from -0.125 to 0.125
- up_scale: float32 [5632], P(('tp', 'fs')), may hold values from 0.5 to 2
- channel_taps: float32 [3, 5632], P(None, 'tp'), may hold values from -3.5 to 3.5
- channel_bias: float32 [5632], P('tp'), may hold values from -3 to 3
- down_weight: float32 [5632, 2048], P('tp', 'fs'), may hold values from -0.078125 to 0.078125
- down_scale: float32 [2048], P('fs'), may hold values from 0.5 to 2
Outputs:
- result: bfloat16 [5120, 2048], P(('rep', 'fs'), 'tp')
The draws below stay inside these ranges and needn't reach their ends.
All inputs are finite; a program needn't handle non-finite values.
Results may differ from the reference program's by a relative error of at most 0.015.
Values may be sent and summed in bfloat16 or wider, within the bound.
No kernel may reach another device: no remote copies, remote signals or barrier semaphores. Data moves between devices by JAX's collectives and lax.ppermute only.
A program may use at most 128 MiB of HBM per device.

```python
import math
import jax
import jax.numpy as jnp
from jax import lax

D = 2048
CW = 1024
FF = 5632
TAPS = 3
LEN = 320
TOKENS = 5120
N_TP = 2


def draw_tokens(key, part):
    first_key, second_key, third_key = jax.random.split(jax.random.fold_in(key, 11), 3)
    rough = jnp.exp(jax.random.uniform(second_key, (D,), jnp.float32, -0.7, 0.7))
    row_scale = jnp.exp(jax.random.uniform(third_key, (TOKENS, 1), jnp.float32, math.log(0.3), math.log(3.0)))
    rising = jnp.exp(jnp.linspace(0.0, math.log(3.0), D)).astype(jnp.float32)
    values = jax.random.normal(first_key, (TOKENS, D), jnp.float32) * row_scale * rough * rising
    return jnp.clip(values, -30.0, 30.0).astype(jnp.bfloat16)


def block_levels(stream_key, extent, cuts, smallest, top_value):
    level, own = 1.0, jax.random.fold_in(stream_key, 6)
    for axis_at, blocks in cuts:
        draws = jnp.exp(jax.random.uniform(jax.random.fold_in(own, axis_at), (blocks,), jnp.float32, smallest / len(cuts), top_value / len(cuts)))
        level = level * jnp.repeat(draws, extent[axis_at] // blocks).reshape([-1 if axis == axis_at else 1 for axis in range(len(extent))])
    return level


def centred(stream_key, extent, spread, most, cuts=(), held_as=jnp.bfloat16):
    result = spread * jax.random.normal(stream_key, extent, jnp.float32)
    if cuts:
        result = result * block_levels(stream_key, extent, cuts, -0.22, 0.18)
    return jnp.clip(result, -most, most).astype(held_as)


def setup_inputs(seed: int = 0) -> dict:
    arg_keys = jax.random.split(jax.random.key(seed), 21)
    return {
        "tokens": draw_tokens(jax.random.fold_in(arg_keys[20], 71), 0),
        "mixer_gain": jnp.clip(1.0 + 0.18 * jax.random.normal(arg_keys[1], (D,), jnp.float32), 0.1, 1.9),
        "outer_weight": centred(arg_keys[2], (D, CW), D ** -0.5, 0.125, ((0, 8), (1, 2)), jnp.float32),
        "inner_weight": centred(arg_keys[3], (D, CW), D ** -0.5, 0.125, ((0, 8), (1, 2)), jnp.float32),
        "value_weight": centred(arg_keys[4], (D, CW), D ** -0.5, 0.125, ((0, 8), (1, 2)), jnp.float32),
        "outer_scale": jnp.clip(jnp.exp(math.log(2.0) - 1.3862944 * jax.random.uniform(arg_keys[5], (CW,), jnp.float32) ** block_levels(arg_keys[5], (CW,), ((0, 16),), -0.2, 0.2)), 0.5, 2.0),
        "inner_scale": jnp.clip(jnp.exp(math.log(2.0) - 1.3862944 * jax.random.uniform(arg_keys[6], (CW,), jnp.float32) ** block_levels(arg_keys[6], (CW,), ((0, 16),), -0.2, 0.2)), 0.5, 2.0),
        "value_scale": jnp.clip(jnp.exp(math.log(2.0) - 1.3862944 * jax.random.uniform(arg_keys[7], (CW,), jnp.float32) ** block_levels(arg_keys[7], (CW,), ((0, 16),), -0.2, 0.2)), 0.5, 2.0),
        "mixer_taps": centred(arg_keys[8], (TAPS, CW), TAPS ** -0.5, 3.5, ((1, 2),), jnp.float32),
        "mixer_project": centred(arg_keys[9], (CW, D), CW ** -0.5, 0.1875, ((0, 2), (1, 8)), jnp.float32),
        "project_scale": jnp.clip(jnp.exp(math.log(2.0) - 1.3862944 * jax.random.uniform(arg_keys[10], (D,), jnp.float32) ** block_levels(arg_keys[10], (D,), ((0, 8),), -0.2, 0.2)), 0.5, 2.0),
        "channel_gain": jnp.clip(1.0 + 0.18 * jax.random.normal(arg_keys[11], (D,), jnp.float32), 0.1, 1.9),
        "gate_weight": centred(arg_keys[12], (D, FF), D ** -0.5, 0.125, ((0, 8), (1, 2)), jnp.float32),
        "gate_scale": jnp.clip(jnp.exp(math.log(2.0) - 1.3862944 * jax.random.uniform(arg_keys[13], (FF,), jnp.float32) ** block_levels(arg_keys[13], (FF,), ((0, 16),), -0.2, 0.2)), 0.5, 2.0),
        "up_weight": centred(arg_keys[14], (D, FF), D ** -0.5, 0.125, ((0, 8), (1, 2)), jnp.float32),
        "up_scale": jnp.clip(jnp.exp(math.log(2.0) - 1.3862944 * jax.random.uniform(arg_keys[15], (FF,), jnp.float32) ** block_levels(arg_keys[15], (FF,), ((0, 16),), -0.2, 0.2)), 0.5, 2.0),
        "channel_taps": centred(arg_keys[16], (TAPS, FF), TAPS ** -0.5, 3.5, ((1, 2),), jnp.float32),
        "channel_bias": centred(arg_keys[17], (FF,), 0.5, 3.0, ((0, 2),), jnp.float32),
        "down_weight": centred(arg_keys[18], (FF, D), FF ** -0.5, 0.078125, ((0, 2), (1, 8)), jnp.float32),
        "down_scale": jnp.clip(jnp.exp(math.log(2.0) - 1.3862944 * jax.random.uniform(arg_keys[19], (D,), jnp.float32) ** block_levels(arg_keys[19], (D,), ((0, 8),), -0.2, 0.2)), 0.5, 2.0),
    }


epsilon = 1e-06

def normalize(token_rows, gain):
    values = token_rows.astype(jnp.float32)
    inverse = lax.rsqrt(lax.optimization_barrier(jnp.sum(values * values, axis=1, keepdims=True)) / values.shape[1] + epsilon)
    return (values * inverse * gain.astype(jnp.float32)).astype(jnp.bfloat16)

def causal_taps(values, taps):
    tap_count = taps.shape[0]
    length = values.shape[0]
    padded = jnp.pad(values, ((tap_count - 1, 0), (0, 0)))
    running = jnp.zeros_like(values)
    for offset in range(tap_count):
        running = running + taps[offset].astype(jnp.float32) * padded[offset:offset + length]
    return running

def block_sums(hidden, weight, scale, blocks):
    length, channels = hidden.shape
    pieces = hidden.reshape(length, blocks, channels // blocks).astype(jnp.float32)
    matrices = weight.reshape(blocks, channels // blocks, weight.shape[1]).astype(jnp.float32)
    partials = jnp.einsum('lbc,bcd->bld', pieces, matrices) * scale.astype(jnp.float32)
    rounded = lax.optimization_barrier(partials.astype(jnp.bfloat16))
    return lax.optimization_barrier(jnp.sum(rounded.astype(jnp.float32), axis=0))

def scaled_product(normed, weight, scale):
    return jnp.dot(normed, weight, preferred_element_type=jnp.float32) * scale.astype(jnp.float32)

def reference(tokens, mixer_gain, outer_weight, inner_weight, value_weight, outer_scale, inner_scale, value_scale, mixer_taps, mixer_project, project_scale, channel_gain, gate_weight, gate_scale, up_weight, up_scale, channel_taps, channel_bias, down_weight, down_scale):
    outer_low = outer_weight.astype(jnp.bfloat16)
    inner_low = inner_weight.astype(jnp.bfloat16)
    value_low = value_weight.astype(jnp.bfloat16)
    project_low = mixer_project.astype(jnp.bfloat16)
    gate_low = gate_weight.astype(jnp.bfloat16)
    up_low = up_weight.astype(jnp.bfloat16)
    down_low = down_weight.astype(jnp.bfloat16)

    def one_sequence(token_rows):
        normed = normalize(token_rows, mixer_gain)
        outer_part = scaled_product(normed, outer_low, outer_scale)
        inner_part = scaled_product(normed, inner_low, inner_scale)
        value_part = scaled_product(normed, value_low, value_scale)
        mixed = (outer_part * causal_taps(inner_part * value_part, mixer_taps)).astype(jnp.bfloat16)
        middle = (token_rows.astype(jnp.float32) + block_sums(mixed, project_low, project_scale, N_TP)).astype(jnp.bfloat16)
        normed_two = normalize(middle, channel_gain)
        gate_part = scaled_product(normed_two, gate_low, gate_scale)
        up_part = scaled_product(normed_two, up_low, up_scale)
        hidden = (jax.nn.silu(causal_taps(gate_part, channel_taps) + channel_bias.astype(jnp.float32)) * up_part).astype(jnp.bfloat16)
        return (middle.astype(jnp.float32) + block_sums(hidden, down_low, down_scale, N_TP)).astype(jnp.bfloat16)
    sequences = tokens.reshape(tokens.shape[0] // LEN, LEN, tokens.shape[1])
    return lax.map(one_sequence, sequences).reshape(tokens.shape)
```

```python
import jax
import jax.numpy as jnp
from jax import lax
from jax.sharding import PartitionSpec as P

LEN = 320

epsilon = 1e-06


def bits_of(count):
    return [1 << at for at in range(count.bit_length() - 1)]


def swap_blocks(values, mask, blocks):
    width = values.shape[-1] // blocks
    return jnp.concatenate(
        [values[..., (p ^ mask) * width : ((p ^ mask) + 1) * width] for p in range(blocks)], axis=-1
    )


def relative_blocks(values, place, blocks):
    for bit in bits_of(blocks):
        values = jnp.where((place & bit) != 0, swap_blocks(values, bit, blocks), values)
    return values


def causal_taps(values, taps):
    tap_count = taps.shape[0]
    grouped = values.reshape(-1, LEN, values.shape[1])
    padded = jnp.pad(grouped, ((0, 0), (tap_count - 1, 0), (0, 0)))
    running = jnp.zeros_like(grouped)
    for offset in range(tap_count):
        running = running + taps[offset] * padded[:, offset : offset + LEN]
    return running.reshape(values.shape)


def per_device(
    tokens,
    mixer_gain,
    outer_weight,
    inner_weight,
    value_weight,
    outer_scale,
    inner_scale,
    value_scale,
    mixer_taps,
    mixer_project,
    project_scale,
    channel_gain,
    gate_weight,
    gate_scale,
    up_weight,
    up_scale,
    channel_taps,
    channel_bias,
    down_weight,
    down_scale,
):
    n_rep, n_fs, n_tp = (lax.axis_size(name) for name in ("rep", "fs", "tp"))
    rep_at, fs_at, tp_at = (lax.axis_index(name) for name in ("rep", "fs", "tp"))
    team = n_rep * 2
    place = rep_at * 2 + (fs_at & 1)
    group = n_fs // n_tp
    high = fs_at // group
    rows = tokens.shape[0]

    def over_fs(values, mask):
        return lax.ppermute(values, "fs", [(at, at ^ mask) for at in range(n_fs)])

    def to_mate(values, mate, core_of=None):
        pairs = []
        for rep in range(n_rep):
            for fs in range(n_fs):
                for tp in range(n_tp):
                    if core_of is not None and core_of(fs) != tp:
                        continue
                    other = ((rep ^ (mate >> 1)) * n_fs + (fs ^ (mate & 1))) * n_tp + tp
                    pairs.append(((rep * n_fs + fs) * n_tp + tp, other))
        return lax.ppermute(values, ("rep", "fs", "tp"), pairs)

    def spread(part):
        blocks = {0: part(place), 1: over_fs(part(place ^ 1), 1)}
        for bit in reversed(bits_of(n_fs)[1:]):
            for at in list(blocks):
                blocks[at ^ bit] = over_fs(blocks[at], bit)
        return [blocks[at] for at in range(n_fs)]

    def columns(weight, at):
        width = weight.shape[1] // team
        return lax.dynamic_slice_in_dim(weight, at * width, width, axis=1).astype(jnp.bfloat16)

    def scaled_rows(weight, scale, at):
        width = weight.shape[0] // team
        return (lax.dynamic_slice_in_dim(weight, at * width, width, axis=0) * scale).astype(jnp.bfloat16)

    def normalize(values, gain):
        squares = lax.psum(jnp.sum(values * values, axis=1), "tp")
        inverse = lax.rsqrt(squares / (values.shape[1] * n_tp) + epsilon)
        return (values * inverse[:, None] * gain).astype(jnp.bfloat16)

    def team_rows(local):
        local = relative_blocks(local, fs_at & (group - 1), group)
        pieces = [local]
        for mate in range(1, team):
            pieces.append(to_mate(swap_blocks(local, 1, group) if mate & 1 else local, mate))
        mine = jnp.concatenate(pieces, axis=0)
        halves = [mine] + [
            lax.ppermute(mine, "tp", [(at, at ^ mask) for at in range(n_tp)]) for mask in range(1, n_tp)
        ]
        first = tp_at ^ high
        if n_tp == 2:
            ordered = [jnp.where(first == 0, halves[0], halves[1]), jnp.where(first == 0, halves[1], halves[0])]
        else:
            stacked = jnp.stack(halves)
            ordered = [lax.dynamic_index_in_dim(stacked, first ^ at, 0, keepdims=False) for at in range(n_tp)]
        return jnp.concatenate(ordered, axis=1)

    def project_back(hidden, blocks):
        results = []
        for at in range(n_tp):
            weight = jnp.concatenate(blocks[at * group : (at + 1) * group], axis=1)
            part = jnp.dot(hidden, weight, preferred_element_type=jnp.float32).astype(jnp.bfloat16)

            def core_of(fs, at=at):
                return (fs // group) ^ at

            if n_tp == 2:
                pairs = [
                    ((lead * 2 + 1 - core_of(lead % n_fs)), (lead * 2 + core_of(lead % n_fs)))
                    for lead in range(n_rep * n_fs)
                ]
                other = lax.ppermute(part, ("rep", "fs", "tp"), pairs)
                whole = part.astype(jnp.float32) + other.astype(jnp.float32)
            else:
                whole = lax.psum(part, "tp").astype(jnp.float32)
            total = whole[:rows]
            for mate in range(1, team):
                piece = to_mate(whole[mate * rows : (mate + 1) * rows].astype(jnp.bfloat16), mate, core_of)
                total = total + (swap_blocks(piece, 1, group) if mate & 1 else piece).astype(jnp.float32)
            results.append(total)
        mine = results[0]
        for at in range(1, n_tp):
            mine = jnp.where((tp_at ^ high) == at, results[at], mine)
        return relative_blocks(mine, fs_at & (group - 1), group)

    widths = [scale.shape[0] for scale in (outer_scale, inner_scale, value_scale, gate_scale, up_scale)]
    known = jnp.concatenate([outer_scale, inner_scale, value_scale, gate_scale, up_scale])[None]
    for bit in bits_of(n_fs):
        known = jnp.concatenate([known, over_fs(known, bit)])
    spans = n_fs // team
    wanted = [
        lax.dynamic_index_in_dim(known, fs_at ^ (place * spans + at), 0, keepdims=False) for at in range(spans)
    ]
    scales, start = [], 0
    for width in widths:
        scales.append(jnp.concatenate([row[start : start + width] for row in wanted]))
        start += width

    mixer_blocks = spread(
        lambda at: jnp.concatenate(
            [columns(weight, at) for weight in (outer_weight, inner_weight, value_weight)], axis=1
        )
    )
    token_values = tokens.astype(jnp.float32)
    normed = team_rows(normalize(token_values, mixer_gain))
    project_blocks = spread(lambda at: scaled_rows(mixer_project, project_scale, at))
    gate_blocks = spread(lambda at: columns(gate_weight, at))
    up_blocks = spread(lambda at: columns(up_weight, at))
    down_blocks = spread(lambda at: scaled_rows(down_weight, down_scale, at))

    def own_columns(values):
        width = values.shape[-1] // team
        return lax.dynamic_slice_in_dim(values, place * width, width, axis=values.ndim - 1)

    parts = jnp.dot(normed, jnp.concatenate(mixer_blocks, axis=0), preferred_element_type=jnp.float32)
    width = parts.shape[1] // 3
    outer_part, inner_part, value_part = (
        parts[:, at * width : (at + 1) * width] * scales[at] for at in range(3)
    )
    mixed = (outer_part * causal_taps(inner_part * value_part, own_columns(mixer_taps))).astype(jnp.bfloat16)
    middle = (token_values + project_back(mixed, project_blocks)).astype(jnp.bfloat16).astype(jnp.float32)
    normed_two = team_rows(normalize(middle, channel_gain))
    gate_part = (
        jnp.dot(normed_two, jnp.concatenate(gate_blocks, axis=0), preferred_element_type=jnp.float32) * scales[3]
    )
    up_part = jnp.dot(normed_two, jnp.concatenate(up_blocks, axis=0), preferred_element_type=jnp.float32) * scales[4]
    hidden = (
        jax.nn.silu(causal_taps(gate_part, own_columns(channel_taps)) + own_columns(channel_bias)) * up_part
    ).astype(jnp.bfloat16)
    return (middle + project_back(hidden, down_blocks)).astype(jnp.bfloat16)


def solution(mesh):
    placed = (
        P(("rep", "fs"), "tp"),
        P("tp"),
        P("fs", "tp"),
        P("fs", "tp"),
        P("fs", "tp"),
        P(("tp", "fs")),
        P(("tp", "fs")),
        P(("tp", "fs")),
        P(None, "tp"),
        P("tp", "fs"),
        P("fs"),
        P("tp"),
        P("fs", "tp"),
        P(("tp", "fs")),
        P("fs", "tp"),
        P(("tp", "fs")),
        P(None, "tp"),
        P("tp"),
        P("tp", "fs"),
        P("fs"),
    )
    return jax.shard_map(
        per_device, mesh=mesh, in_specs=placed, out_specs=P(("rep", "fs"), "tp"), check_vma=False
    )
```
